32 devices in a mesh: fs: 8 (over z, x), tp: 4 (over y, core).
Axes of the slice: x: 2, y: 2, z: 4, core: 2. Of those that a mesh axis runs over, the one named last changes fastest.
Arguments:
- saved_input: bfloat16 [2048, 4096], P('fs'), may hold values from -8 to 8
- query_cotangent: bfloat16 [2048, 2048], P('fs', 'tp'), may hold values from -6 to 6
- layer_cotangent: bfloat16 [2048, 4096], P('fs'), may hold values from -8 to 8
- mixed_heads: bfloat16 [2048, 2048], P('fs', 'tp'), may hold values from -6 to 6
- query_basis: bfloat16 [4096, 256], P('fs'), may hold values from -0.125 to 0.125
- output_basis: bfloat16 [4096, 256], P('fs'), may hold values from -0.125 to 0.125
- query_master: float32 [4096, 2048], P('fs', 'tp'), may hold values from -3 to 3
- output_master: float32 [4096, 2048], P('fs', 'tp'), may hold values from -3 to 3
- query_first: float32 [256, 2048], P('fs', 'tp'), may hold values from -6 to 6
- query_second: float32 [256, 2048], P('fs', 'tp'), may hold values from 0.25 to 4
- output_first: float32 [256, 2048], P('fs', 'tp'), may hold values from -6 to 6
- output_second: float32 [256, 2048], P('fs', 'tp'), may hold values from 0.25 to 4
Outputs:
- query_weight: float32 [4096, 2048], P('fs', 'tp')
- output_weight: float32 [4096, 2048], P('fs', 'tp')
- query_step: float32 [4096, 2048], P('fs', 'tp')
- output_step: float32 [4096, 2048], P('fs', 'tp')
- query_first_new: float32 [256, 2048], P('fs', 'tp')
- query_second_new: float32 [256, 2048], P('fs', 'tp')
- output_first_new: float32 [256, 2048], P('fs', 'tp')
- output_second_new: float32 [256, 2048], P('fs', 'tp')
- query_copy: bfloat16 [4096, 2048], P(None, 'tp')
- output_copy: bfloat16 [4096, 2048], P(None, 'tp')
The draws below stay inside these ranges and needn't reach their ends.
All inputs are finite; a program needn't handle non-finite values.
Results may differ from the reference program's by a relative error of at most 0.0028.
Values may be sent and summed in bfloat16 or wider, within the bound.
A program may use at most 64 MiB of HBM per device.

```python
import math
import jax
import jax.numpy as jnp
from jax import lax

D = 4096
QW = 2048
RANK = 256
TOKENS = 2048


def with_spikes(values, rng, source, target, parts, factor):
    owner, partner = [(jnp.arange(values.shape[axis_at]) // (values.shape[axis_at] // parts)).reshape([-1 if axis == axis_at else 1 for axis in range(values.ndim)]) for axis_at in (source, target)]
    chosen = jax.random.permutation(rng, parts)[partner]
    strong = (owner == chosen) | (owner == (partner + parts // 2) % parts)
    return jnp.where(strong, factor * values, values)


def block_scale(rng, dims, shards, smallest, high):
    factor_of, own = 1.0, jax.random.fold_in(rng, 6)
    for dim, shards_of in shards:
        draws = jnp.exp(jax.random.uniform(jax.random.fold_in(own, dim), (shards_of,), jnp.float32, smallest / len(shards), high / len(shards)))
        factor_of = factor_of * jnp.repeat(draws, dims[dim] // shards_of).reshape([-1 if axis == dim else 1 for axis in range(len(dims))])
    return factor_of


def centred(stream_key, shape, scale, reach, shards=(), kind=jnp.bfloat16):
    drawn = scale * jax.random.normal(stream_key, shape, jnp.float32)
    if shards:
        drawn = drawn * block_scale(stream_key, shape, shards, -0.22, 0.18)
    return jnp.clip(drawn, -reach, reach).astype(kind)


def bell_draw_with(rng, shape, spread, limit, cuts, heavy, held_as=jnp.bfloat16):
    values = spread * jax.random.normal(rng, shape, jnp.float32)
    if cuts:
        values = values * block_scale(rng, shape, cuts, -0.22, 0.18)
    return jnp.clip(with_spikes(values, jax.random.fold_in(rng, 3), *heavy), -limit, limit).astype(held_as)


def setup_inputs(seed: int = 0) -> dict:
    key_of = jax.random.split(jax.random.key(seed), 13)
    saved_input = bell_draw_with(key_of[0], (TOKENS, D), 1.0, 8.0, ((0, 8),), (0, 1, 8, 2.0))
    query_cotangent = centred(key_of[1], (TOKENS, QW), 1.0, 6.0, ((0, 8), (1, 4)))
    layer_cotangent = bell_draw_with(key_of[2], (TOKENS, D), 1.0, 8.0, ((0, 8),), (0, 1, 8, 2.0))
    mixed_heads = centred(key_of[3], (TOKENS, QW), 1.0, 6.0, ((0, 8), (1, 4)))
    query_basis = bell_draw_with(key_of[4], (D, RANK), D ** -0.5, 0.125, ((0, 8),), (0, 1, 8, 2.0))
    output_basis = bell_draw_with(key_of[5], (D, RANK), D ** -0.5, 0.125, ((0, 8),), (0, 1, 8, 2.0))
    query_master = centred(key_of[6], (D, QW), 0.5, 3.0, ((0, 8), (1, 4)), jnp.float32)
    output_master = centred(key_of[7], (D, QW), 0.5, 3.0, ((0, 8), (1, 4)), jnp.float32)
    query_first = centred(key_of[8], (RANK, QW), 1.0, 6.0, ((0, 8), (1, 4)), jnp.float32)
    query_second = jnp.clip(jnp.exp(math.log(4.0) - 2.7725887 * jax.random.uniform(key_of[9], (RANK, QW), jnp.float32) ** block_scale(key_of[9], (RANK, QW), ((0, 8), (1, 4)), -0.2, 0.2)), 0.25, 4.0)
    output_first = centred(key_of[10], (RANK, QW), 1.0, 6.0, ((0, 8), (1, 4)), jnp.float32)
    output_second = jnp.clip(jnp.exp(math.log(4.0) - 2.7725887 * jax.random.uniform(key_of[11], (RANK, QW), jnp.float32) ** block_scale(key_of[11], (RANK, QW), ((0, 8), (1, 4)), -0.2, 0.2)), 0.25, 4.0)
    return dict(saved_input=saved_input, query_cotangent=query_cotangent, layer_cotangent=layer_cotangent, mixed_heads=mixed_heads, query_basis=query_basis, output_basis=output_basis, query_master=query_master, output_master=output_master, query_first=query_first, query_second=query_second, output_first=output_first, output_second=output_second)


beta_one = 0.8
beta_two = 0.9
rate = 0.1

def projected_gradient(saved, cotangent, basis):
    gradient = jnp.dot(saved.T, cotangent, preferred_element_type=jnp.float32)
    return jnp.dot(basis.astype(jnp.float32).T, gradient, precision=lax.Precision.HIGHEST)

def moment_update(low, factor, first, second):
    scaled = low * factor
    first_new = beta_one * first + (1.0 - beta_one) * scaled
    second_new = beta_two * second + (1.0 - beta_two) * scaled * scaled
    direction = (first_new / jnp.sqrt(second_new)).astype(jnp.bfloat16)
    return (first_new, second_new, direction)

def reference(saved_input, query_cotangent, layer_cotangent, mixed_heads, query_basis, output_basis, query_master, output_master, query_first, query_second, output_first, output_second):
    query_low = projected_gradient(saved_input, query_cotangent, query_basis)
    output_low = projected_gradient(layer_cotangent, mixed_heads, output_basis)
    meansq = (jnp.sum(query_low * query_low) + jnp.sum(output_low * output_low)) / (2.0 * RANK * QW)
    factor = 1.0 / jnp.sqrt(1.0 + meansq)
    qf, qs, qdir = moment_update(query_low, factor, query_first, query_second)
    of, osec, odir = moment_update(output_low, factor, output_first, output_second)
    query_step = jnp.dot(query_basis, qdir, preferred_element_type=jnp.float32)
    output_step = jnp.dot(output_basis, odir, preferred_element_type=jnp.float32)
    query_weight = query_master - rate * query_step
    output_weight = output_master - rate * output_step
    return (query_weight, output_weight, query_step, output_step, qf, qs, of, osec, query_weight.astype(jnp.bfloat16), output_weight.astype(jnp.bfloat16))
```

```python
import functools

import jax
import jax.numpy as jnp
from jax import lax
from jax.experimental import pallas as pl
from jax.experimental.pallas import tpu as pltpu
from jax.sharding import PartitionSpec as P

QW = 2048
RANK = 256


beta_one = 0.8
beta_two = 0.9
rate = 0.1


def moment_update(low, factor, first, second):
    scaled = low * factor
    first_new = beta_one * first + (1.0 - beta_one) * scaled
    second_new = beta_two * second + (1.0 - beta_two) * scaled * scaled
    direction = (first_new / jnp.sqrt(second_new)).astype(jnp.bfloat16)
    return (first_new, second_new, direction)


def contract_tokens(left, right):
    return lax.dot_general(
        left,
        right,
        (((0,), (0,)), ((), ())),
        precision=lax.Precision.HIGHEST,
        preferred_element_type=jnp.float32,
    )


def per_device(
    saved_input,
    query_cotangent,
    layer_cotangent,
    mixed_heads,
    query_basis,
    output_basis,
    query_master,
    output_master,
    query_first,
    query_second,
    output_first,
    output_second,
):
    query_coords = jnp.dot(
        saved_input,
        lax.all_gather(query_basis, "fs", axis=0, tiled=True),
        preferred_element_type=jnp.float32,
    )
    output_coords = jnp.dot(
        layer_cotangent,
        lax.all_gather(output_basis, "fs", axis=0, tiled=True),
        preferred_element_type=jnp.float32,
    )
    query_part = contract_tokens(query_coords, query_cotangent.astype(jnp.float32))
    output_part = contract_tokens(output_coords, mixed_heads.astype(jnp.float32))
    query_low, output_low = (
        lax.psum_scatter(query_part, "fs", scatter_dimension=0, tiled=True),
        lax.psum_scatter(output_part, "fs", scatter_dimension=0, tiled=True),
    )
    local_squares = jnp.sum(query_low * query_low) + jnp.sum(output_low * output_low)
    total_squares = lax.psum(local_squares, ("fs", "tp"))
    factor = 1.0 / jnp.sqrt(1.0 + total_squares / (2.0 * RANK * QW))
    qf, qs, qdir = moment_update(query_low, factor, query_first, query_second)
    of, osec, odir = moment_update(output_low, factor, output_first, output_second)
    query_whole, output_whole = (
        lax.all_gather(qdir, "fs", axis=0, tiled=True),
        lax.all_gather(odir, "fs", axis=0, tiled=True),
    )
    query_step = jnp.dot(query_basis, query_whole, preferred_element_type=jnp.float32)
    output_step = jnp.dot(output_basis, output_whole, preferred_element_type=jnp.float32)
    query_weight = query_master - rate * query_step
    output_weight = output_master - rate * output_step
    query_copy, output_copy = (
        lax.all_gather(query_weight.astype(jnp.bfloat16), "fs", axis=0, tiled=True),
        lax.all_gather(output_weight.astype(jnp.bfloat16), "fs", axis=0, tiled=True),
    )
    return (
        query_weight,
        output_weight,
        query_step,
        output_step,
        qf,
        qs,
        of,
        osec,
        query_copy,
        output_copy,
    )

MESH = pl.DeviceIdType.MESH
CHUNKS = 4


def ring_kernel(n, m, *refs):
    x_hbm, cot_hbm, basis, master_hbm, first, second = (
        (refs[0], refs[2]),
        (refs[1], refs[3]),
        (refs[4], refs[5]),
        (refs[6], refs[7]),
        (refs[8], refs[10]),
        (refs[9], refs[11]),
    )
    w_out, step_out, first_out, second_out, copy_out = (
        (refs[12], refs[13]),
        (refs[14], refs[15]),
        (refs[16], refs[18]),
        (refs[17], refs[19]),
        (refs[20], refs[21]),
    )
    (
        x_v, cot_v, master_v, mine_v, rows_v, coord_v, part_v, got_v, square_v, direction_v, w_v, step_v, gather_v,
        in_sem, out_sem, local_sem, rows_sem, coord_sem, part_sem, square_sem, direction_sem, gather_sem,
    ) = refs[22:]
    f, t = lax.axis_index("fs"), lax.axis_index("tp")
    me = f * m + t
    rank_part = mine_v.shape[1]
    block = basis[0].shape[0]
    low_rows = first[0].shape[0]
    rank = basis[0].shape[1]

    loads = {}
    for k in range(2):
        loads["x", k] = pltpu.make_async_copy(x_hbm[k], x_v.at[k], in_sem.at[k])
        loads["cot", k] = pltpu.make_async_copy(cot_hbm[k], cot_v.at[k], in_sem.at[2 + k])
        loads["master", k] = pltpu.make_async_copy(master_hbm[k], master_v.at[k], in_sem.at[4 + k])
    for copy in loads.values():
        copy.start()

    barrier = pltpu.get_barrier_semaphore()
    for d in range(1, n * m):
        other = lax.rem(me + d, n * m)
        pl.semaphore_signal(barrier, inc=1, device_id={"fs": other // m, "tp": lax.rem(other, m)}, device_id_type=MESH)

    chosen = lax.broadcasted_iota(jnp.int32, (rank_part, rank), 1) == (
        lax.broadcasted_iota(jnp.int32, (rank_part, rank), 0) + t * rank_part
    )
    select = jnp.where(chosen, 1.0, 0.0).astype(jnp.bfloat16)
    for k in range(2):
        mine_v[k] = lax.dot_general(
            select, basis[k][...], (((1,), (1,)), ((), ())), preferred_element_type=jnp.float32
        ).astype(jnp.bfloat16)
    pl.semaphore_wait(barrier, n * m - 1)

    def remote(source, target, sems, index, device):
        return pltpu.make_async_remote_copy(
            src_ref=source,
            dst_ref=target,
            send_sem=sems.at[(0,) + index],
            recv_sem=sems.at[(1,) + index],
            device_id=device,
            device_id_type=MESH,
        )

    sent = []
    rows = {}
    for k in range(2):
        for d in range(1, n):
            rows[k, d] = remote(mine_v.at[k], rows_v.at[k, d], rows_sem, (k, d), {"fs": lax.rem(f + d, n)})
            rows[k, d].start()
            sent.append(rows[k, d])

    parts = {}
    for k in range(2):
        loads["x", k].wait()
        total = jnp.zeros((rank_part, x_v.shape[1]), jnp.float32)
        for d in range(n):
            if d > 0:
                rows[k, d].wait_recv()
            source = lax.rem(f - d + n, n)
            left = mine_v[k] if d == 0 else rows_v[k, d]
            right = x_v[k, :, pl.ds(pl.multiple_of(source * block, block), block)]
            total = total + lax.dot_general(left, right, (((1,), (1,)), ((), ())), preferred_element_type=jnp.float32)
        high = total.astype(jnp.bfloat16)
        coord_v[k, t, 0] = high
        coord_v[k, t, 1] = (total - high.astype(jnp.float32)).astype(jnp.bfloat16)
        coords = []
        for d in range(1, m):
            copy = remote(coord_v.at[k, t], coord_v.at[k, t], coord_sem, (k, d), {"tp": lax.rem(t + d, m)})
            copy.start()
            coords.append(copy)
            sent.append(copy)
        loads["cot", k].wait()
        for copy in coords:
            copy.wait_recv()
        whole_high = coord_v[k, :, 0].reshape(rank, x_v.shape[1])
        whole_low = coord_v[k, :, 1].reshape(rank, x_v.shape[1])
        part = jnp.dot(whole_high, cot_v[k], preferred_element_type=jnp.float32) + jnp.dot(
            whole_low, cot_v[k], preferred_element_type=jnp.float32
        )
        part_v[k] = part.reshape(n, low_rows, part.shape[1])
        for d in range(1, n):
            other = lax.rem(f + d, n)
            parts[k, d] = remote(part_v.at[k, other], got_v.at[k, d], part_sem, (k, d), {"fs": other})
            parts[k, d].start()
            sent.append(parts[k, d])

    lows = []
    squares = jnp.zeros((), jnp.float32)
    for k in range(2):
        low = part_v[k, f]
        for d in range(1, n):
            parts[k, d].wait_recv()
            low = low + got_v[k, d]
        lows.append(low)
        squares = squares + jnp.sum(low * low)
    square_v[0] = jnp.full(square_v.shape[1:], squares, jnp.float32)
    copies = []
    for d in range(1, n * m):
        other = lax.rem(me + d, n * m)
        copy = remote(
            square_v.at[0], square_v.at[d], square_sem, (d,), {"fs": other // m, "tp": lax.rem(other, m)}
        )
        copy.start()
        copies.append(copy)
        sent.append(copy)
    for copy in copies:
        copy.wait_recv()
    total_squares = jnp.sum(square_v[...], axis=0)[:1, :1]
    factor = 1.0 / jnp.sqrt(1.0 + total_squares / (2.0 * rank * (first[0].shape[1] * m)))

    directions = []
    for k in range(2):
        new_first, new_second, direction = moment_update(lows[k], factor, first[k][...], second[k][...])
        first_out[k][...] = new_first
        second_out[k][...] = new_second
        direction_v[k, f] = direction
        for d in range(1, n):
            copy = remote(
                direction_v.at[k, f], direction_v.at[k, f], direction_sem, (k, d), {"fs": lax.rem(f + d, n)}
            )
            copy.start()
            directions.append(copy)
            sent.append(copy)

    half = n // 2
    z, x = f // 2, lax.rem(f, 2)
    place = (1 - x) * z + x * (n - 1 - z)

    def at(p):
        p = lax.rem(p + 2 * n, n)
        h = p // half
        return (1 - h) * 2 * p + h * (2 * (n - 1 - p) + 1)

    toward = (at(place + 1), at(place - 1))
    origin = [[at(place - s), at(place + s)] for s in range(n)]
    piece = block // CHUNKS
    wholes = []
    for k in range(2):
        loads["master", k].wait()
        for copy in directions[k * (n - 1) : (k + 1) * (n - 1)]:
            copy.wait_recv()
    local = []
    ring = {}

    def forward(s, k, c):
        where = gather_v.at[k, origin[s][k], pl.ds(c * piece, piece)]
        if s < n - 1:
            ring[s, k, c] = remote(where, where, gather_sem, (k, s, c), {"fs": toward[k]})
            ring[s, k, c].start()
            sent.append(ring[s, k, c])
        copy = pltpu.make_async_copy(
            where,
            copy_out[k].at[pl.ds(pl.multiple_of(origin[s][k] * block + c * piece, piece), piece)],
            local_sem.at[k, s, c],
        )
        copy.start()
        local.append(copy)

    for c in range(CHUNKS):
        for k in range(2):
            span = pl.ds(c * piece, piece)
            step = jnp.dot(
                basis[k][span, :],
                direction_v[k].reshape(rank, direction_v.shape[3]),
                preferred_element_type=jnp.float32,
            )
            weight = master_v[k, span, :] - rate * step
            gather_v[k, f, span] = weight.astype(jnp.bfloat16)
            forward(0, k, c)
            step_v[k, span] = step
            w_v[k, span] = weight
    for k in range(2):
        for i, (source, target) in enumerate(((w_v, w_out), (step_v, step_out))):
            copy = pltpu.make_async_copy(source.at[k], target[k], out_sem.at[i, k])
            copy.start()
            local.append(copy)
    for s in range(1, n):
        for c in range(CHUNKS):
            for k in range(2):
                ring[s - 1, k, c].wait_recv()
                forward(s, k, c)
    for copy in sent:
        copy.wait_send()
    for copy in local:
        copy.wait()


def fused_per_device(n, m, *args):
    x, cot, _, _, basis = args[:5]
    first = args[8]
    block, rank = basis.shape
    columns = cot.shape[1]
    tokens, width = x.shape
    part = rank // m
    low_rows = first.shape[0]
    big = jax.ShapeDtypeStruct((block, columns), jnp.float32)
    small = jax.ShapeDtypeStruct(first.shape, jnp.float32)
    copied = jax.ShapeDtypeStruct((width, columns), jnp.bfloat16)
    hbm = pl.BlockSpec(memory_space=pl.ANY)
    vmem = pl.BlockSpec(memory_space=pltpu.VMEM)
    bf16, f32 = jnp.bfloat16, jnp.float32
    dma = pltpu.SemaphoreType.DMA
    return pl.pallas_call(
        functools.partial(ring_kernel, n, m),
        out_shape=(big,) * 4 + (small,) * 4 + (copied,) * 2,
        in_specs=[hbm] * 4 + [vmem] * 2 + [hbm] * 2 + [vmem] * 4,
        out_specs=(hbm,) * 4 + (vmem,) * 4 + (hbm,) * 2,
        scratch_shapes=[
            pltpu.VMEM((2, tokens, width), bf16),
            pltpu.VMEM((2, tokens, columns), bf16),
            pltpu.VMEM((2, block, columns), f32),
            pltpu.VMEM((2, part, block), bf16),
            pltpu.VMEM((2, n, part, block), bf16),
            pltpu.VMEM((2, m, 2, part, tokens), bf16),
            pltpu.VMEM((2, n, low_rows, columns), f32),
            pltpu.VMEM((2, n, low_rows, columns), f32),
            pltpu.VMEM((n * m, 8, 128), f32),
            pltpu.VMEM((2, n, low_rows, columns), bf16),
            pltpu.VMEM((2, block, columns), f32),
            pltpu.VMEM((2, block, columns), f32),
            pltpu.VMEM((2, n, block, columns), bf16),
            dma((6,)),
            dma((2, 2)),
            dma((2, n, CHUNKS)),
            dma((2, 2, n)),
            dma((2, 2, m)),
            dma((2, 2, n)),
            dma((2, n * m)),
            dma((2, 2, n)),
            dma((2, 2, n - 1, CHUNKS)),
        ],
        compiler_params=pltpu.CompilerParams(
            collective_id=0, has_side_effects=True, vmem_limit_bytes=50 * 2**20
        ),
    )(*args)


def fits(n, m, *args):
    basis, first = args[4], args[8]
    return (
        n % 2 == 0
        and basis.shape[1] // n % 16 == 0
        and basis.shape[1] // m % 16 == 0
        and basis.shape[0] // n % (16 * CHUNKS) == 0
        and basis.shape[0] // n % 128 == 0
        and first.shape[1] // m % 128 == 0
    )


def solution(mesh):
    placed = (
        P("fs", None),
        P("fs", "tp"),
        P("fs", None),
        P("fs", "tp"),
        P("fs", None),
        P("fs", None),
        P("fs", "tp"),
        P("fs", "tp"),
        P("fs", "tp"),
        P("fs", "tp"),
        P("fs", "tp"),
        P("fs", "tp"),
    )
    n, m = mesh.shape["fs"], mesh.shape["tp"]

    def step(*args):
        body = functools.partial(fused_per_device, n, m) if fits(n, m, *args) else per_device
        return jax.shard_map(
            body,
            mesh=mesh,
            in_specs=placed,
            out_specs=(P("fs", "tp"),) * 8 + (P(None, "tp"),) * 2,
            check_vma=False,
        )(*args)

    return step
```

```python
import functools

import jax
import jax.numpy as jnp
from jax import lax
from jax.experimental import pallas as pl
from jax.experimental.pallas import tpu as pltpu
from jax.sharding import PartitionSpec as P

QW = 2048
RANK = 256


beta_one = 0.8
beta_two = 0.9
rate = 0.1


def moment_update(low, factor, first, second):
    scaled = low * factor
    first_new = beta_one * first + (1.0 - beta_one) * scaled
    second_new = beta_two * second + (1.0 - beta_two) * scaled * scaled
    direction = (first_new / jnp.sqrt(second_new)).astype(jnp.bfloat16)
    return (first_new, second_new, direction)


def contract_tokens(left, right):
    return lax.dot_general(
        left,
        right,
        (((0,), (0,)), ((), ())),
        precision=lax.Precision.HIGHEST,
        preferred_element_type=jnp.float32,
    )


def per_device(
    saved_input,
    query_cotangent,
    layer_cotangent,
    mixed_heads,
    query_basis,
    output_basis,
    query_master,
    output_master,
    query_first,
    query_second,
    output_first,
    output_second,
):
    query_coords = jnp.dot(
        saved_input,
        lax.all_gather(query_basis, "fs", axis=0, tiled=True),
        preferred_element_type=jnp.float32,
    )
    output_coords = jnp.dot(
        layer_cotangent,
        lax.all_gather(output_basis, "fs", axis=0, tiled=True),
        preferred_element_type=jnp.float32,
    )
    query_part = contract_tokens(query_coords, query_cotangent.astype(jnp.float32))
    output_part = contract_tokens(output_coords, mixed_heads.astype(jnp.float32))
    query_low, output_low = (
        lax.psum_scatter(query_part, "fs", scatter_dimension=0, tiled=True),
        lax.psum_scatter(output_part, "fs", scatter_dimension=0, tiled=True),
    )
    local_squares = jnp.sum(query_low * query_low) + jnp.sum(output_low * output_low)
    total_squares = lax.psum(local_squares, ("fs", "tp"))
    factor = 1.0 / jnp.sqrt(1.0 + total_squares / (2.0 * RANK * QW))
    qf, qs, qdir = moment_update(query_low, factor, query_first, query_second)
    of, osec, odir = moment_update(output_low, factor, output_first, output_second)
    query_whole, output_whole = (
        lax.all_gather(qdir, "fs", axis=0, tiled=True),
        lax.all_gather(odir, "fs", axis=0, tiled=True),
    )
    query_step = jnp.dot(query_basis, query_whole, preferred_element_type=jnp.float32)
    output_step = jnp.dot(output_basis, output_whole, preferred_element_type=jnp.float32)
    query_weight = query_master - rate * query_step
    output_weight = output_master - rate * output_step
    query_copy, output_copy = (
        lax.all_gather(query_weight.astype(jnp.bfloat16), "fs", axis=0, tiled=True),
        lax.all_gather(output_weight.astype(jnp.bfloat16), "fs", axis=0, tiled=True),
    )
    return (
        query_weight,
        output_weight,
        query_step,
        output_step,
        qf,
        qs,
        of,
        osec,
        query_copy,
        output_copy,
    )

MESH = pl.DeviceIdType.MESH
CHUNKS = 4


def ring_kernel(n, m, *refs):
    x_hbm, cot_hbm, basis_hbm, master_hbm, first_hbm, second_hbm = (
        (refs[0], refs[2]),
        (refs[1], refs[3]),
        (refs[4], refs[5]),
        (refs[6], refs[7]),
        (refs[8], refs[10]),
        (refs[9], refs[11]),
    )
    w_out, step_out, first_out, second_out, gathered = (
        (refs[12], refs[13]),
        (refs[14], refs[15]),
        (refs[16], refs[18]),
        (refs[17], refs[19]),
        (refs[20], refs[21]),
    )
    (
        x_v, cot_v, basis, master_v, first, second,
        mine_v, rows_v, coord_v, part_v, pair_v, got_v, square_v, direction_v,
        in_sem, rows_sem, coord_sem, pair_sem, part_sem, square_sem, direction_sem, gather_sem,
    ) = refs[22:]
    f, t = lax.axis_index("fs"), lax.axis_index("tp")
    me = f * m + t
    rank_part, block = mine_v.shape[1:]
    rank = basis.shape[2]
    tokens = x_v.shape[1]
    columns = cot_v.shape[2]
    low_rows = first.shape[1]
    half = n // 2
    z, x = f // 2, lax.rem(f, 2)
    across = z * 2 + 1 - x

    def along(d, side=None):
        side = x if side is None else side
        return lax.rem(z + d + half, half) * 2 + side

    loads = {}
    for k in range(2):
        loads["basis", k] = pltpu.make_async_copy(basis_hbm[k], basis.at[k], in_sem.at[0, k])
    for i, (name, sources, target) in enumerate(
        (
            ("x", x_hbm, x_v),
            ("cot", cot_hbm, cot_v),
            ("first", first_hbm, first),
            ("second", second_hbm, second),
            ("master", master_hbm, master_v),
        )
    ):
        for k in range(2):
            loads[name, k] = pltpu.make_async_copy(sources[k], target.at[k], in_sem.at[1 + i, k])
    for copy in loads.values():
        copy.start()

    barrier = pltpu.get_barrier_semaphore()
    for d in range(1, n * m):
        other = lax.rem(me + d, n * m)
        pl.semaphore_signal(barrier, inc=1, device_id={"fs": other // m, "tp": lax.rem(other, m)}, device_id_type=MESH)

    chosen = lax.broadcasted_iota(jnp.int32, (rank_part, rank), 1) == (
        lax.broadcasted_iota(jnp.int32, (rank_part, rank), 0) + t * rank_part
    )
    select = jnp.where(chosen, 1.0, 0.0).astype(jnp.bfloat16)
    for k in range(2):
        loads["basis", k].wait()
        mine_v[k] = lax.dot_general(
            select, basis[k], (((1,), (1,)), ((), ())), preferred_element_type=jnp.float32
        ).astype(jnp.bfloat16)
    pl.semaphore_wait(barrier, n * m - 1)

    sent = []

    def send(source, target, sems, index, device):
        copy = pltpu.make_async_remote_copy(
            src_ref=source,
            dst_ref=target,
            send_sem=sems.at[(0,) + index],
            recv_sem=sems.at[(1,) + index],
            device_id=device,
            device_id_type=MESH,
        )
        copy.start()
        sent.append(copy)
        return copy

    def push(own, slots, sems, k):
        copies = {half: send(own, slots(half), sems, (k, half), {"fs": across})}
        for d in (1, half - 1, *range(2, half - 1)):
            copies[d] = send(own, slots(d), sems, (k, d), {"fs": along(d)})
        return copies

    def relay(copies, slots, sems, k):
        for d in (1, half - 1, *range(2, half - 1)):
            copies[d].wait_recv()
            copies[half + d] = send(slots(d), slots(half + d), sems, (k, half + d), {"fs": across})

    def rows_at(k):
        return lambda d: rows_v.at[k, d]

    rows = [push(mine_v.at[k], rows_at(k), rows_sem, k) for k in range(2)]

    def coordinates(k, d):
        source = along(-(d % half), x if d < half else 1 - x)
        left = mine_v[k] if d == 0 else rows_v[k, d]
        right = x_v[k, :, pl.ds(pl.multiple_of(source * block, block), block)]
        return lax.dot_general(left, right, (((1,), (1,)), ((), ())), preferred_element_type=jnp.float32)

    coords = []
    for k in range(2):
        if k == 0:
            relay(rows[0], rows_at(0), rows_sem, 0)
        loads["x", k].wait()
        total = coordinates(k, 0)
        for d in range(1, half):
            total = total + coordinates(k, d)
        if k == 0:
            relay(rows[1], rows_at(1), rows_sem, 1)
        for d in range(half, n):
            rows[k][d].wait_recv()
            total = total + coordinates(k, d)
        high = total.astype(jnp.bfloat16)
        coord_v[k, t, 0] = high
        coord_v[k, t, 1] = (total - high.astype(jnp.float32)).astype(jnp.bfloat16)
        coords.append(
            [
                send(coord_v.at[k, t], coord_v.at[k, t], coord_sem, (k, d), {"tp": lax.rem(t + d, m)})
                for d in range(1, m)
            ]
        )

    pairs = []
    for k in range(2):
        loads["cot", k].wait()
        for copy in coords[k]:
            copy.wait_recv()
        part = jnp.dot(
            coord_v[k, :, 0].reshape(rank, tokens), cot_v[k], preferred_element_type=jnp.float32
        ) + jnp.dot(coord_v[k, :, 1].reshape(rank, tokens), cot_v[k], preferred_element_type=jnp.float32)
        part_v[k] = part.reshape(n, low_rows, columns)
        pairs.append({})
        for d in (1, half - 1, *range(2, half - 1), 0):
            pairs[k][d] = send(
                part_v.at[k, along(d, 1 - x)], pair_v.at[k, d], pair_sem, (k, d), {"fs": across}
            )
    parts = []
    for k in range(2):
        parts.append({})
        for d in (1, half - 1, *range(2, half - 1)):
            pairs[k][d].wait_recv()
            pair_v[k, d] = pair_v[k, d] + part_v[k, along(d)]
            parts[k][d] = send(pair_v.at[k, d], got_v.at[k, d], part_sem, (k, d), {"fs": along(d)})

    lows = []
    squares = jnp.zeros((), jnp.float32)
    for k in range(2):
        pairs[k][0].wait_recv()
        low = pair_v[k, 0] + part_v[k, f]
        for d in range(1, half):
            parts[k][d].wait_recv()
            low = low + got_v[k, d]
        lows.append(low)
        squares = squares + jnp.sum(low * low)
    square_v[0] = jnp.full(square_v.shape[1:], squares, jnp.float32)
    copies = []
    for d in range(1, n * m):
        other = lax.rem(me + d, n * m)
        copies.append(
            send(square_v.at[0], square_v.at[d], square_sem, (d,), {"fs": other // m, "tp": lax.rem(other, m)})
        )
    for k in range(2):
        loads["first", k].wait()
        loads["second", k].wait()
    for copy in copies:
        copy.wait_recv()
    total_squares = jnp.sum(square_v[...], axis=0)[:1, :1]
    factor = 1.0 / jnp.sqrt(1.0 + total_squares / (2.0 * rank * (columns * m)))

    directions = []
    for k in range(2):
        new_first, new_second, direction = moment_update(lows[k], factor, first[k], second[k])
        direction_v[k, f] = direction
        own = direction_v.at[k, f]
        directions.append(push(own, lambda d: own, direction_sem, k))
        first_out[k][...] = new_first
        second_out[k][...] = new_second
    for k in range(2):
        for d in (1, half - 1, *range(2, half - 1)):
            directions[k][d].wait_recv()
            arrived = direction_v.at[k, along(-d)]
            directions[k][half + d] = send(arrived, arrived, direction_sem, (k, half + d), {"fs": across})

    place = (1 - x) * z + x * (n - 1 - z)

    def at(p):
        p = lax.rem(p + 2 * n, n)
        h = p // half
        return (1 - h) * 2 * p + h * (2 * (n - 1 - p) + 1)

    toward = (at(place + 1), at(place - 1))
    origin = [[at(place - s), at(place + s)] for s in range(n)]
    piece = block // CHUNKS
    for k in range(2):
        loads["master", k].wait()
        for d in range(half, n):
            directions[k][d].wait_recv()
    ring = {}

    def forward(s, k, c):
        where = gathered[k].at[pl.ds(pl.multiple_of(origin[s][k] * block + c * piece, piece), piece)]
        ring[s, k, c] = send(where, where, gather_sem, (k, s, c), {"fs": toward[k]})

    for c in range(CHUNKS):
        for k in range(2):
            span = pl.ds(c * piece, piece)
            step = jnp.dot(
                basis[k, span, :],
                direction_v[k].reshape(rank, columns),
                preferred_element_type=jnp.float32,
            )
            weight = master_v[k, span, :] - rate * step
            gathered[k][pl.ds(pl.multiple_of(f * block + c * piece, piece), piece)] = weight.astype(jnp.bfloat16)
            forward(0, k, c)
            step_out[k][span] = step
            w_out[k][span] = weight
    for s in range(1, n):
        for c in range(CHUNKS):
            for k in range(2):
                ring[s - 1, k, c].wait_recv()
                if s < n - 1:
                    forward(s, k, c)
    for copy in sent:
        copy.wait_send()


def write_kernel(count, *refs):
    sem = refs[2 * count]
    copies = [pltpu.make_async_copy(refs[i], refs[count + i], sem.at[i]) for i in range(count)]
    for copy in copies:
        copy.start()
    for copy in copies:
        copy.wait()


def fused_per_device(n, m, *args):
    x, cot, _, _, basis = args[:5]
    first = args[8]
    block, rank = basis.shape
    columns = cot.shape[1]
    tokens, width = x.shape
    part = rank // m
    low_rows = first.shape[0]
    bf16, f32 = jnp.bfloat16, jnp.float32
    kinds = [((block, columns), f32)] * 4 + [(first.shape, f32)] * 4 + [((width, columns), bf16)] * 2
    hbm = pl.BlockSpec(memory_space=pltpu.HBM)
    vmem = pl.BlockSpec(memory_space=pltpu.VMEM)
    dma = pltpu.SemaphoreType.DMA
    results = pl.pallas_call(
        functools.partial(ring_kernel, n, m),
        out_shape=tuple(pltpu.VMEM(*kind) for kind in kinds),
        in_specs=[hbm] * 12,
        out_specs=(vmem,) * 10,
        scratch_shapes=[
            pltpu.VMEM((2, tokens, width), bf16),
            pltpu.VMEM((2, tokens, columns), bf16),
            pltpu.VMEM((2, block, rank), bf16),
            pltpu.VMEM((2, block, columns), f32),
            pltpu.VMEM((2, low_rows, columns), f32),
            pltpu.VMEM((2, low_rows, columns), f32),
            pltpu.VMEM((2, part, block), bf16),
            pltpu.VMEM((2, n, part, block), bf16),
            pltpu.VMEM((2, m, 2, part, tokens), bf16),
            pltpu.VMEM((2, n, low_rows, columns), f32),
            pltpu.VMEM((2, n // 2, low_rows, columns), f32),
            pltpu.VMEM((2, n // 2, low_rows, columns), f32),
            pltpu.VMEM((n * m, 8, 128), f32),
            pltpu.VMEM((2, n, low_rows, columns), bf16),
            dma((6, 2)),
            dma((2, 2, n)),
            dma((2, 2, m)),
            dma((2, 2, n // 2)),
            dma((2, 2, n // 2)),
            dma((2, n * m)),
            dma((2, 2, n)),
            dma((2, 2, n - 1, CHUNKS)),
        ],
        compiler_params=pltpu.CompilerParams(
            collective_id=0, has_side_effects=True, vmem_limit_bytes=48 * 2**20
        ),
    )(*args)
    return pl.pallas_call(
        functools.partial(write_kernel, len(kinds)),
        out_shape=tuple(jax.ShapeDtypeStruct(*kind) for kind in kinds),
        in_specs=[pl.BlockSpec(memory_space=pl.ANY)] * len(kinds),
        out_specs=(hbm,) * len(kinds),
        scratch_shapes=[dma((len(kinds),))],
        compiler_params=pltpu.CompilerParams(vmem_limit_bytes=2**20),
    )(*results)


def fits(n, m, *args):
    basis, first = args[4], args[8]
    return (
        n % 2 == 0
        and basis.shape[1] // n % 16 == 0
        and basis.shape[1] // m % 16 == 0
        and basis.shape[0] // n % (16 * CHUNKS) == 0
        and basis.shape[0] // n % 128 == 0
        and first.shape[1] // m % 128 == 0
    )


def solution(mesh):
    placed = (
        P("fs", None),
        P("fs", "tp"),
        P("fs", None),
        P("fs", "tp"),
        P("fs", None),
        P("fs", None),
        P("fs", "tp"),
        P("fs", "tp"),
        P("fs", "tp"),
        P("fs", "tp"),
        P("fs", "tp"),
        P("fs", "tp"),
    )
    n, m = mesh.shape["fs"], mesh.shape["tp"]

    def step(*args):
        body = functools.partial(fused_per_device, n, m) if fits(n, m, *args) else per_device
        return jax.shard_map(
            body,
            mesh=mesh,
            in_specs=placed,
            out_specs=(P("fs", "tp"),) * 8 + (P(None, "tp"),) * 2,
            check_vma=False,
        )(*args)

    return step
```

```python
import functools

import jax
import jax.numpy as jnp
from jax import lax
from jax.experimental import pallas as pl
from jax.experimental.pallas import tpu as pltpu
from jax.sharding import PartitionSpec as P

QW = 2048
RANK = 256


beta_one = 0.8
beta_two = 0.9
rate = 0.1


def moment_update(low, factor, first, second):
    scaled = low * factor
    first_new = beta_one * first + (1.0 - beta_one) * scaled
    second_new = beta_two * second + (1.0 - beta_two) * scaled * scaled
    direction = (first_new / jnp.sqrt(second_new)).astype(jnp.bfloat16)
    return (first_new, second_new, direction)


def contract_tokens(left, right):
    return lax.dot_general(
        left,
        right,
        (((0,), (0,)), ((), ())),
        precision=lax.Precision.HIGHEST,
        preferred_element_type=jnp.float32,
    )


def per_device(
    saved_input,
    query_cotangent,
    layer_cotangent,
    mixed_heads,
    query_basis,
    output_basis,
    query_master,
    output_master,
    query_first,
    query_second,
    output_first,
    output_second,
):
    query_coords = jnp.dot(
        saved_input,
        lax.all_gather(query_basis, "fs", axis=0, tiled=True),
        preferred_element_type=jnp.float32,
    )
    output_coords = jnp.dot(
        layer_cotangent,
        lax.all_gather(output_basis, "fs", axis=0, tiled=True),
        preferred_element_type=jnp.float32,
    )
    query_part = contract_tokens(query_coords, query_cotangent.astype(jnp.float32))
    output_part = contract_tokens(output_coords, mixed_heads.astype(jnp.float32))
    query_low, output_low = (
        lax.psum_scatter(query_part, "fs", scatter_dimension=0, tiled=True),
        lax.psum_scatter(output_part, "fs", scatter_dimension=0, tiled=True),
    )
    local_squares = jnp.sum(query_low * query_low) + jnp.sum(output_low * output_low)
    total_squares = lax.psum(local_squares, ("fs", "tp"))
    factor = 1.0 / jnp.sqrt(1.0 + total_squares / (2.0 * RANK * QW))
    qf, qs, qdir = moment_update(query_low, factor, query_first, query_second)
    of, osec, odir = moment_update(output_low, factor, output_first, output_second)
    query_whole, output_whole = (
        lax.all_gather(qdir, "fs", axis=0, tiled=True),
        lax.all_gather(odir, "fs", axis=0, tiled=True),
    )
    query_step = jnp.dot(query_basis, query_whole, preferred_element_type=jnp.float32)
    output_step = jnp.dot(output_basis, output_whole, preferred_element_type=jnp.float32)
    query_weight = query_master - rate * query_step
    output_weight = output_master - rate * output_step
    query_copy, output_copy = (
        lax.all_gather(query_weight.astype(jnp.bfloat16), "fs", axis=0, tiled=True),
        lax.all_gather(output_weight.astype(jnp.bfloat16), "fs", axis=0, tiled=True),
    )
    return (
        query_weight,
        output_weight,
        query_step,
        output_step,
        qf,
        qs,
        of,
        osec,
        query_copy,
        output_copy,
    )

MESH = pl.DeviceIdType.MESH
CHUNKS = 4


def ring_kernel(n, m, *refs):
    x_hbm, cot_hbm, basis_hbm, master_hbm, first_hbm, second_hbm = (
        (refs[0], refs[2]),
        (refs[1], refs[3]),
        (refs[4], refs[5]),
        (refs[6], refs[7]),
        (refs[8], refs[10]),
        (refs[9], refs[11]),
    )
    w_out, step_out, first_out, second_out, gathered = (
        (refs[12], refs[13]),
        (refs[14], refs[15]),
        (refs[16], refs[18]),
        (refs[17], refs[19]),
        (refs[20], refs[21]),
    )
    (
        x_v, cot_v, basis, master_v, first, second,
        rows_v, ahead_v, wide_v, coord_v, part_v, pair_v, got_v, square_v, direction_v,
        in_sem, rows_sem, coord_sem, pair_sem, part_sem, square_sem, direction_sem, gather_sem, ahead_sem, wide_sem,
    ) = refs[22:]
    f, t = lax.axis_index("fs"), lax.axis_index("tp")
    me = f * m + t
    rank_part, block = rows_v.shape[2:]
    piece = block // CHUNKS
    rank = basis.shape[2]
    tokens = x_v.shape[1]
    columns = cot_v.shape[2]
    low_rows = first.shape[1]
    half = n // 2
    z, x = f // 2, lax.rem(f, 2)
    across = z * 2 + 1 - x

    def along(d, side=None):
        side = x if side is None else side
        return lax.rem(z + d + half, half) * 2 + side

    loads = {}
    for k in range(2):
        loads["basis", k] = pltpu.make_async_copy(basis_hbm[k], basis.at[k], in_sem.at[0, k])
    for i, (name, sources, target) in enumerate(
        (
            ("x", x_hbm, x_v),
            ("cot", cot_hbm, cot_v),
            ("first", first_hbm, first),
            ("second", second_hbm, second),
            ("master", master_hbm, master_v),
        )
    ):
        for k in range(2):
            loads[name, k] = pltpu.make_async_copy(sources[k], target.at[k], in_sem.at[1 + i, k])
    for copy in loads.values():
        copy.start()

    barrier = pltpu.get_barrier_semaphore()
    for d in range(1, n * m):
        other = lax.rem(me + d, n * m)
        pl.semaphore_signal(barrier, inc=1, device_id={"fs": other // m, "tp": lax.rem(other, m)}, device_id_type=MESH)

    chosen = lax.broadcasted_iota(jnp.int32, (rank_part, rank), 1) == (
        lax.broadcasted_iota(jnp.int32, (rank_part, rank), 0) + t * rank_part
    )
    select = jnp.where(chosen, 1.0, 0.0).astype(jnp.bfloat16)
    for k in range(2):
        loads["basis", k].wait()
        rows_v[k, 0] = lax.dot_general(
            select, basis[k], (((1,), (1,)), ((), ())), preferred_element_type=jnp.float32
        ).astype(jnp.bfloat16)
    pl.semaphore_wait(barrier, n * m - 1)

    sent = []

    def send(source, target, sems, index, device):
        copy = pltpu.make_async_remote_copy(
            src_ref=source,
            dst_ref=target,
            send_sem=sems.at[(0,) + index],
            recv_sem=sems.at[(1,) + index],
            device_id=device,
            device_id_type=MESH,
        )
        copy.start()
        sent.append(copy)
        return copy

    def push(own, slots, sems, k):
        copies = {half: send(own, slots(half), sems, (k, half), {"fs": across})}
        for d in (1, half - 1, *range(2, half - 1)):
            copies[d] = send(own, slots(d), sems, (k, d), {"fs": along(d)})
        return copies

    def relay(copies, slots, sems, k):
        for d in (1, half - 1, *range(2, half - 1)):
            copies[d].wait_recv()
            copies[half + d] = send(slots(d), slots(half + d), sems, (k, half + d), {"fs": across})

    def rows_at(k):
        return lambda d: rows_v.at[k, d]

    rows = [push(rows_v.at[k, 0], rows_at(k), rows_sem, k) for k in range(2)]

    def coordinates(k, d):
        source = along(-(d % half), x if d < half else 1 - x)
        left = rows_v[k, d]
        right = x_v[k, :, pl.ds(pl.multiple_of(source * block, block), block)]
        return lax.dot_general(left, right, (((1,), (1,)), ((), ())), preferred_element_type=jnp.float32)

    def ahead_at(k):
        return lambda d: ahead_v.at[k, d]

    coords, ahead = [], []
    for k in range(2):
        if k == 0:
            relay(rows[0], rows_at(0), rows_sem, 0)
        loads["x", k].wait()
        total = coordinates(k, 0)
        for d in range(1, half):
            total = total + coordinates(k, d)
        if k == 0:
            relay(rows[1], rows_at(1), rows_sem, 1)
            for i in range(2):
                loads["master", i].wait()
                ahead_v[i, 0] = master_v[i, pl.ds(0, piece)].astype(jnp.bfloat16)
                ahead.append(push(ahead_v.at[i, 0], ahead_at(i), ahead_sem, i))
        for d in range(half, n):
            rows[k][d].wait_recv()
            total = total + coordinates(k, d)
        high = total.astype(jnp.bfloat16)
        coord_v[k, t, 0] = high
        coord_v[k, t, 1] = (total - high.astype(jnp.float32)).astype(jnp.bfloat16)
        coords.append(
            [
                send(coord_v.at[k, t], coord_v.at[k, t], coord_sem, (k, d), {"tp": lax.rem(t + d, m)})
                for d in range(1, m)
            ]
        )

    wide = []
    for k in range(2):
        source = rows_v.at[k, :, :, pl.ds(0, piece)]
        for d in range(1, m):
            wide.append(send(source, wide_v.at[k, t], wide_sem, (k, d), {"tp": lax.rem(t + d, m)}))
        wide_v[k, t] = rows_v[k, :, :, :piece]
    pairs = []
    for k in range(2):
        loads["cot", k].wait()
        for copy in coords[k]:
            copy.wait_recv()
        part = jnp.dot(
            coord_v[k, :, 0].reshape(rank, tokens), cot_v[k], preferred_element_type=jnp.float32
        ) + jnp.dot(coord_v[k, :, 1].reshape(rank, tokens), cot_v[k], preferred_element_type=jnp.float32)
        part_v[k] = part.reshape(n, low_rows, columns)
        pairs.append({})
        for d in (1, half - 1, *range(2, half - 1), 0):
            pairs[k][d] = send(
                part_v.at[k, along(d, 1 - x)], pair_v.at[k, d], pair_sem, (k, d), {"fs": across}
            )
    parts = []
    for k in range(2):
        relay(ahead[k], ahead_at(k), ahead_sem, k)
        parts.append({})
        for d in (1, half - 1, *range(2, half - 1)):
            pairs[k][d].wait_recv()
            pair_v[k, d] = pair_v[k, d] + part_v[k, along(d)]
            parts[k][d] = send(pair_v.at[k, d], got_v.at[k, d], part_sem, (k, d), {"fs": along(d)})

    lows = []
    squares = jnp.zeros((), jnp.float32)
    for k in range(2):
        pairs[k][0].wait_recv()
        low = pair_v[k, 0] + part_v[k, f]
        for d in range(1, half):
            parts[k][d].wait_recv()
            low = low + got_v[k, d]
        lows.append(low)
        squares = squares + jnp.sum(low * low)
    square_v[0] = jnp.full(square_v.shape[1:], squares, jnp.float32)
    copies = []
    for d in range(1, n * m):
        other = lax.rem(me + d, n * m)
        copies.append(
            send(square_v.at[0], square_v.at[d], square_sem, (d,), {"fs": other // m, "tp": lax.rem(other, m)})
        )
    for k in range(2):
        loads["first", k].wait()
        loads["second", k].wait()
    for copy in copies:
        copy.wait_recv()
    total_squares = jnp.sum(square_v[...], axis=0)[:1, :1]
    factor = 1.0 / jnp.sqrt(1.0 + total_squares / (2.0 * rank * (columns * m)))

    directions = []
    for k in range(2):
        new_first, new_second, direction = moment_update(lows[k], factor, first[k], second[k])
        direction_v[k, f] = direction
        own = direction_v.at[k, f]
        directions.append(push(own, lambda d: own, direction_sem, k))
        first_out[k][...] = new_first
        second_out[k][...] = new_second
    for k in range(2):
        for d in (1, half - 1, *range(2, half - 1)):
            directions[k][d].wait_recv()
            arrived = direction_v.at[k, along(-d)]
            directions[k][half + d] = send(arrived, arrived, direction_sem, (k, half + d), {"fs": across})

    place = (1 - x) * z + x * (n - 1 - z)

    def at(p):
        p = lax.rem(p + 2 * n, n)
        h = p // half
        return (1 - h) * 2 * p + h * (2 * (n - 1 - p) + 1)

    toward = (at(place + 1), at(place - 1))
    origin = [[at(place - s), at(place + s)] for s in range(n)]
    for k in range(2):
        for d in range(half, n):
            directions[k][d].wait_recv()
    ring = {}

    def forward(s, k, c):
        where = gathered[k].at[pl.ds(pl.multiple_of(origin[s][k] * block + c * piece, piece), piece)]
        ring[s, k, c] = send(where, where, gather_sem, (k, s, c), {"fs": toward[k]})

    def own_piece(c):
        for k in range(2):
            span = pl.ds(c * piece, piece)
            step = jnp.dot(
                basis[k, span, :],
                direction_v[k].reshape(rank, columns),
                preferred_element_type=jnp.float32,
            )
            weight = master_v[k, span, :] - rate * step
            if c > 0:
                gathered[k][pl.ds(pl.multiple_of(f * block + c * piece, piece), piece)] = weight.astype(jnp.bfloat16)
                forward(0, k, c)
            step_out[k][span] = step
            w_out[k][span] = weight
    def finish_ahead(d):
        source = along(-(d % half), x if d < half else 1 - x)
        for k in range(2):
            step = lax.dot_general(
                wide_v[k, :, d].reshape(rank, piece),
                direction_v[k].reshape(rank, columns),
                (((0,), (0,)), ((), ())),
                preferred_element_type=jnp.float32,
            )
            weight = ahead_v[k, d].astype(jnp.float32) - rate * step
            gathered[k][pl.ds(pl.multiple_of(source * block, block), piece)] = weight.astype(jnp.bfloat16)

    for c in (*range(1, CHUNKS), 0):
        own_piece(c)
    for copy in wide:
        copy.wait_recv()
    for k in range(2):
        for d in range(half, n):
            ahead[k][d].wait_recv()
    finish_ahead(0)
    for s in range(1, n):
        for c in range(1, CHUNKS):
            for k in range(2):
                ring[s - 1, k, c].wait_recv()
                if s < n - 1:
                    forward(s, k, c)
        finish_ahead(s)
    for copy in sent:
        copy.wait_send()


def write_kernel(count, *refs):
    sem = refs[2 * count]
    copies = [pltpu.make_async_copy(refs[i], refs[count + i], sem.at[i]) for i in range(count)]
    for copy in copies:
        copy.start()
    for copy in copies:
        copy.wait()


def fused_per_device(n, m, *args):
    x, cot, _, _, basis = args[:5]
    first = args[8]
    block, rank = basis.shape
    columns = cot.shape[1]
    tokens, width = x.shape
    part = rank // m
    low_rows = first.shape[0]
    bf16, f32 = jnp.bfloat16, jnp.float32
    kinds = [((block, columns), f32)] * 4 + [(first.shape, f32)] * 4 + [((width, columns), bf16)] * 2
    hbm = pl.BlockSpec(memory_space=pltpu.HBM)
    vmem = pl.BlockSpec(memory_space=pltpu.VMEM)
    dma = pltpu.SemaphoreType.DMA
    results = pl.pallas_call(
        functools.partial(ring_kernel, n, m),
        out_shape=tuple(pltpu.VMEM(*kind) for kind in kinds),
        in_specs=[hbm] * 12,
        out_specs=(vmem,) * 10,
        scratch_shapes=[
            pltpu.VMEM((2, tokens, width), bf16),
            pltpu.VMEM((2, tokens, columns), bf16),
            pltpu.VMEM((2, block, rank), bf16),
            pltpu.VMEM((2, block, columns), f32),
            pltpu.VMEM((2, low_rows, columns), f32),
            pltpu.VMEM((2, low_rows, columns), f32),
            pltpu.VMEM((2, n, part, block), bf16),
            pltpu.VMEM((2, n, block // CHUNKS, columns), bf16),
            pltpu.VMEM((2, m, n, part, block // CHUNKS), bf16),
            pltpu.VMEM((2, m, 2, part, tokens), bf16),
            pltpu.VMEM((2, n, low_rows, columns), f32),
            pltpu.VMEM((2, n // 2, low_rows, columns), f32),
            pltpu.VMEM((2, n // 2, low_rows, columns), f32),
            pltpu.VMEM((n * m, 8, 128), f32),
            pltpu.VMEM((2, n, low_rows, columns), bf16),
            dma((6, 2)),
            dma((2, 2, n)),
            dma((2, 2, m)),
            dma((2, 2, n // 2)),
            dma((2, 2, n // 2)),
            dma((2, n * m)),
            dma((2, 2, n)),
            dma((2, 2, n - 1, CHUNKS)),
            dma((2, 2, n)),
            dma((2, 2, m)),
        ],
        compiler_params=pltpu.CompilerParams(
            collective_id=0, has_side_effects=True, vmem_limit_bytes=48 * 2**20
        ),
    )(*args)
    return pl.pallas_call(
        functools.partial(write_kernel, len(kinds)),
        out_shape=tuple(jax.ShapeDtypeStruct(*kind) for kind in kinds),
        in_specs=[pl.BlockSpec(memory_space=pl.ANY)] * len(kinds),
        out_specs=(hbm,) * len(kinds),
        scratch_shapes=[dma((len(kinds),))],
        compiler_params=pltpu.CompilerParams(vmem_limit_bytes=2**20),
    )(*results)


def fits(n, m, *args):
    basis, first = args[4], args[8]
    return (
        n % 2 == 0
        and basis.shape[1] // n % 16 == 0
        and basis.shape[1] // m % 16 == 0
        and basis.shape[0] // n % (128 * CHUNKS) == 0
        and basis.shape[0] // n % 128 == 0
        and first.shape[1] // m % 128 == 0
    )


def solution(mesh):
    placed = (
        P("fs", None),
        P("fs", "tp"),
        P("fs", None),
        P("fs", "tp"),
        P("fs", None),
        P("fs", None),
        P("fs", "tp"),
        P("fs", "tp"),
        P("fs", "tp"),
        P("fs", "tp"),
        P("fs", "tp"),
        P("fs", "tp"),
    )
    n, m = mesh.shape["fs"], mesh.shape["tp"]

    def step(*args):
        body = functools.partial(fused_per_device, n, m) if fits(n, m, *args) else per_device
        return jax.shard_map(
            body,
            mesh=mesh,
            in_specs=placed,
            out_specs=(P("fs", "tp"),) * 8 + (P(None, "tp"),) * 2,
            check_vma=False,
        )(*args)

    return step
```

```python
import functools

import jax
import jax.numpy as jnp
from jax import lax
from jax.experimental import pallas as pl
from jax.experimental.pallas import tpu as pltpu
from jax.sharding import PartitionSpec as P

QW = 2048
RANK = 256


beta_one = 0.8
beta_two = 0.9
rate = 0.1


def moment_update(low, factor, first, second):
    scaled = low * factor
    first_new = beta_one * first + (1.0 - beta_one) * scaled
    second_new = beta_two * second + (1.0 - beta_two) * scaled * scaled
    direction = (first_new / jnp.sqrt(second_new)).astype(jnp.bfloat16)
    return (first_new, second_new, direction)


def contract_tokens(left, right):
    return lax.dot_general(
        left,
        right,
        (((0,), (0,)), ((), ())),
        precision=lax.Precision.HIGHEST,
        preferred_element_type=jnp.float32,
    )


def per_device(
    saved_input,
    query_cotangent,
    layer_cotangent,
    mixed_heads,
    query_basis,
    output_basis,
    query_master,
    output_master,
    query_first,
    query_second,
    output_first,
    output_second,
):
    query_coords = jnp.dot(
        saved_input,
        lax.all_gather(query_basis, "fs", axis=0, tiled=True),
        preferred_element_type=jnp.float32,
    )
    output_coords = jnp.dot(
        layer_cotangent,
        lax.all_gather(output_basis, "fs", axis=0, tiled=True),
        preferred_element_type=jnp.float32,
    )
    query_part = contract_tokens(query_coords, query_cotangent.astype(jnp.float32))
    output_part = contract_tokens(output_coords, mixed_heads.astype(jnp.float32))
    query_low, output_low = (
        lax.psum_scatter(query_part, "fs", scatter_dimension=0, tiled=True),
        lax.psum_scatter(output_part, "fs", scatter_dimension=0, tiled=True),
    )
    local_squares = jnp.sum(query_low * query_low) + jnp.sum(output_low * output_low)
    total_squares = lax.psum(local_squares, ("fs", "tp"))
    factor = 1.0 / jnp.sqrt(1.0 + total_squares / (2.0 * RANK * QW))
    qf, qs, qdir = moment_update(query_low, factor, query_first, query_second)
    of, osec, odir = moment_update(output_low, factor, output_first, output_second)
    query_whole, output_whole = (
        lax.all_gather(qdir, "fs", axis=0, tiled=True),
        lax.all_gather(odir, "fs", axis=0, tiled=True),
    )
    query_step = jnp.dot(query_basis, query_whole, preferred_element_type=jnp.float32)
    output_step = jnp.dot(output_basis, output_whole, preferred_element_type=jnp.float32)
    query_weight = query_master - rate * query_step
    output_weight = output_master - rate * output_step
    query_copy, output_copy = (
        lax.all_gather(query_weight.astype(jnp.bfloat16), "fs", axis=0, tiled=True),
        lax.all_gather(output_weight.astype(jnp.bfloat16), "fs", axis=0, tiled=True),
    )
    return (
        query_weight,
        output_weight,
        query_step,
        output_step,
        qf,
        qs,
        of,
        osec,
        query_copy,
        output_copy,
    )

MESH = pl.DeviceIdType.MESH
CHUNKS = 4


def ring_kernel(n, m, *refs):
    x_hbm, cot_hbm, basis_hbm, master_hbm, first_hbm, second_hbm = (
        (refs[0], refs[2]),
        (refs[1], refs[3]),
        (refs[4], refs[5]),
        (refs[6], refs[7]),
        (refs[8], refs[10]),
        (refs[9], refs[11]),
    )
    w_out, step_out, first_out, second_out, gathered = (
        (refs[12], refs[13]),
        (refs[14], refs[15]),
        (refs[16], refs[18]),
        (refs[17], refs[19]),
        (refs[20], refs[21]),
    )
    (
        x_v, cot_v, basis, master_v, first, second,
        rows_v, ahead_v, wide_v, flat_v, coord_v, part_v, pair_v, got_v, square_v, direction_v,
        in_sem, rows_sem, coord_sem, pair_sem, part_sem, square_sem, direction_sem, gather_sem, ahead_sem, wide_sem,
    ) = refs[22:]
    f, t = lax.axis_index("fs"), lax.axis_index("tp")
    me = f * m + t
    rank_part, block = rows_v.shape[2:]
    piece = block // CHUNKS
    rank = basis.shape[2]
    tokens = x_v.shape[1]
    columns = cot_v.shape[2]
    low_rows = first.shape[1]
    half = n // 2
    z, x = f // 2, lax.rem(f, 2)
    across = z * 2 + 1 - x

    def along(d, side=None):
        side = x if side is None else side
        return lax.rem(z + d + half, half) * 2 + side

    loads = {}
    for k in range(2):
        loads["basis", k] = pltpu.make_async_copy(basis_hbm[k], basis.at[k], in_sem.at[0, k])
    for i, (name, sources, target) in enumerate(
        (
            ("x", x_hbm, x_v),
            ("cot", cot_hbm, cot_v),
            ("first", first_hbm, first),
            ("second", second_hbm, second),
            ("master", master_hbm, master_v),
        )
    ):
        for k in range(2):
            loads[name, k] = pltpu.make_async_copy(sources[k], target.at[k], in_sem.at[1 + i, k])
    for copy in loads.values():
        copy.start()

    barrier = pltpu.get_barrier_semaphore()
    for d in range(1, n * m):
        other = lax.rem(me + d, n * m)
        pl.semaphore_signal(barrier, inc=1, device_id={"fs": other // m, "tp": lax.rem(other, m)}, device_id_type=MESH)

    chosen = lax.broadcasted_iota(jnp.int32, (rank_part, rank), 1) == (
        lax.broadcasted_iota(jnp.int32, (rank_part, rank), 0) + t * rank_part
    )
    select = jnp.where(chosen, 1.0, 0.0).astype(jnp.bfloat16)
    for k in range(2):
        loads["basis", k].wait()
        rows_v[k, 0] = lax.dot_general(
            select, basis[k], (((1,), (1,)), ((), ())), preferred_element_type=jnp.float32
        ).astype(jnp.bfloat16)
    pl.semaphore_wait(barrier, n * m - 1)

    sent = []

    def send(source, target, sems, index, device):
        copy = pltpu.make_async_remote_copy(
            src_ref=source,
            dst_ref=target,
            send_sem=sems.at[(0,) + index],
            recv_sem=sems.at[(1,) + index],
            device_id=device,
            device_id_type=MESH,
        )
        copy.start()
        sent.append(copy)
        return copy

    def push(own, slots, sems, k):
        copies = {half: send(own, slots(half), sems, (k, half), {"fs": across})}
        for d in (1, half - 1, *range(2, half - 1)):
            copies[d] = send(own, slots(d), sems, (k, d), {"fs": along(d)})
        return copies

    def relay(copies, slots, sems, k):
        for d in (1, half - 1, *range(2, half - 1)):
            copies[d].wait_recv()
            copies[half + d] = send(slots(d), slots(half + d), sems, (k, half + d), {"fs": across})

    def rows_at(k):
        return lambda d: rows_v.at[k, d]

    rows = [push(rows_v.at[k, 0], rows_at(k), rows_sem, k) for k in range(2)]

    def coordinates(k, d):
        source = along(-(d % half), x if d < half else 1 - x)
        left = rows_v[k, d]
        right = x_v[k, :, pl.ds(pl.multiple_of(source * block, block), block)]
        return lax.dot_general(left, right, (((1,), (1,)), ((), ())), preferred_element_type=jnp.float32)

    def ahead_at(k):
        return lambda d: ahead_v.at[k, d]

    coords, ahead = [], []
    for k in range(2):
        if k == 0:
            relay(rows[0], rows_at(0), rows_sem, 0)
        loads["x", k].wait()
        total = coordinates(k, 0)
        for d in range(1, half):
            total = total + coordinates(k, d)
        if k == 0:
            relay(rows[1], rows_at(1), rows_sem, 1)
            for i in range(2):
                loads["master", i].wait()
                ahead_v[i, 0] = master_v[i, pl.ds(0, piece)].astype(jnp.bfloat16)
                ahead.append(push(ahead_v.at[i, 0], ahead_at(i), ahead_sem, i))
        for d in range(half, n):
            rows[k][d].wait_recv()
            total = total + coordinates(k, d)
        high = total.astype(jnp.bfloat16)
        coord_v[k, t, 0] = high
        coord_v[k, t, 1] = (total - high.astype(jnp.float32)).astype(jnp.bfloat16)
        coords.append(
            [
                send(coord_v.at[k, t], coord_v.at[k, t], coord_sem, (k, d), {"tp": lax.rem(t + d, m)})
                for d in range(1, m)
            ]
        )

    wide = []
    for k in range(2):
        source = rows_v.at[k, :, :, pl.ds(0, piece)]
        for d in range(1, m):
            wide.append(send(source, wide_v.at[k, t], wide_sem, (k, d), {"tp": lax.rem(t + d, m)}))
        wide_v[k, t] = rows_v[k, :, :, :piece]
    pairs = []
    for k in range(2):
        loads["cot", k].wait()
        for copy in coords[k]:
            copy.wait_recv()
        part = jnp.dot(
            coord_v[k, :, 0].reshape(rank, tokens), cot_v[k], preferred_element_type=jnp.float32
        ) + jnp.dot(coord_v[k, :, 1].reshape(rank, tokens), cot_v[k], preferred_element_type=jnp.float32)
        part_v[k] = part.reshape(n, low_rows, columns)
        pairs.append({})
        for d in (1, half - 1, *range(2, half - 1), 0):
            pairs[k][d] = send(
                part_v.at[k, along(d, 1 - x)], pair_v.at[k, d], pair_sem, (k, d), {"fs": across}
            )
    parts = []
    for k in range(2):
        relay(ahead[k], ahead_at(k), ahead_sem, k)
        parts.append({})
        for d in (1, half - 1, *range(2, half - 1)):
            pairs[k][d].wait_recv()
            pair_v[k, d] = pair_v[k, d] + part_v[k, along(d)]
            parts[k][d] = send(pair_v.at[k, d], got_v.at[k, d], part_sem, (k, d), {"fs": along(d)})

    lows = []
    squares = jnp.zeros((), jnp.float32)
    for k in range(2):
        pairs[k][0].wait_recv()
        low = pair_v[k, 0] + part_v[k, f]
        for d in range(1, half):
            parts[k][d].wait_recv()
            low = low + got_v[k, d]
        lows.append(low)
        squares = squares + jnp.sum(low * low)
    square_v[0] = jnp.full(square_v.shape[1:], squares, jnp.float32)
    copies = []
    for d in range(1, n * m):
        other = lax.rem(me + d, n * m)
        copies.append(
            send(square_v.at[0], square_v.at[d], square_sem, (d,), {"fs": other // m, "tp": lax.rem(other, m)})
        )
    for copy in wide:
        copy.wait_recv()
    for k in range(2):
        for d in range(n):
            flat_v[k, d] = wide_v[k, :, d].reshape(rank, piece).T
    for k in range(2):
        loads["first", k].wait()
        loads["second", k].wait()
    for copy in copies:
        copy.wait_recv()
    total_squares = jnp.sum(square_v[...], axis=0)[:1, :1]
    factor = 1.0 / jnp.sqrt(1.0 + total_squares / (2.0 * rank * (columns * m)))

    directions = []
    for k in range(2):
        new_first, new_second, direction = moment_update(lows[k], factor, first[k], second[k])
        direction_v[k, f] = direction
        own = direction_v.at[k, f]
        directions.append(push(own, lambda d: own, direction_sem, k))
        first_out[k][...] = new_first
        second_out[k][...] = new_second
    for k in range(2):
        for d in (1, half - 1, *range(2, half - 1)):
            directions[k][d].wait_recv()
            arrived = direction_v.at[k, along(-d)]
            directions[k][half + d] = send(arrived, arrived, direction_sem, (k, half + d), {"fs": across})

    place = (1 - x) * z + x * (n - 1 - z)

    def at(p):
        p = lax.rem(p + 2 * n, n)
        h = p // half
        return (1 - h) * 2 * p + h * (2 * (n - 1 - p) + 1)

    toward = (at(place + 1), at(place - 1))
    origin = [[at(place - s), at(place + s)] for s in range(n)]
    for k in range(2):
        for d in range(half, n):
            directions[k][d].wait_recv()
    ring = {}

    def forward(s, k, c):
        where = gathered[k].at[pl.ds(pl.multiple_of(origin[s][k] * block + c * piece, piece), piece)]
        ring[s, k, c] = send(where, where, gather_sem, (k, s, c), {"fs": toward[k]})

    def own_piece(c):
        for k in range(2):
            span = pl.ds(c * piece, piece)
            step = jnp.dot(
                basis[k, span, :],
                direction_v[k].reshape(rank, columns),
                preferred_element_type=jnp.float32,
            )
            weight = master_v[k, span, :] - rate * step
            if c > 0:
                gathered[k][pl.ds(pl.multiple_of(f * block + c * piece, piece), piece)] = weight.astype(jnp.bfloat16)
                forward(0, k, c)
            step_out[k][span] = step
            w_out[k][span] = weight
    def finish_ahead(k, d):
        source = along(-(d % half), x if d < half else 1 - x)
        if d >= half:
            ahead[k][d].wait_recv()
        step = jnp.dot(
            flat_v[k, d], direction_v[k].reshape(rank, columns), preferred_element_type=jnp.float32
        )
        weight = ahead_v[k, d].astype(jnp.float32) - rate * step
        gathered[k][pl.ds(pl.multiple_of(source * block, block), piece)] = weight.astype(jnp.bfloat16)

    for c in (*range(1, CHUNKS), 0):
        own_piece(c)
    units = [(k, d) for d in range(n) for k in range(2)]
    for s in range(1, n):
        for c in range(1, CHUNKS):
            for k in range(2):
                ring[s - 1, k, c].wait_recv()
                if s < n - 1:
                    forward(s, k, c)
            if units:
                finish_ahead(*units.pop(0))
    for unit in units:
        finish_ahead(*unit)
    for copy in sent:
        copy.wait_send()


def write_kernel(count, *refs):
    sem = refs[2 * count]
    copies = [pltpu.make_async_copy(refs[i], refs[count + i], sem.at[i]) for i in range(count)]
    for copy in copies:
        copy.start()
    for copy in copies:
        copy.wait()


def fused_per_device(n, m, *args):
    x, cot, _, _, basis = args[:5]
    first = args[8]
    block, rank = basis.shape
    columns = cot.shape[1]
    tokens, width = x.shape
    part = rank // m
    low_rows = first.shape[0]
    bf16, f32 = jnp.bfloat16, jnp.float32
    kinds = [((block, columns), f32)] * 4 + [(first.shape, f32)] * 4 + [((width, columns), bf16)] * 2
    hbm = pl.BlockSpec(memory_space=pltpu.HBM)
    vmem = pl.BlockSpec(memory_space=pltpu.VMEM)
    dma = pltpu.SemaphoreType.DMA
    results = pl.pallas_call(
        functools.partial(ring_kernel, n, m),
        out_shape=tuple(pltpu.VMEM(*kind) for kind in kinds),
        in_specs=[hbm] * 12,
        out_specs=(vmem,) * 10,
        scratch_shapes=[
            pltpu.VMEM((2, tokens, width), bf16),
            pltpu.VMEM((2, tokens, columns), bf16),
            pltpu.VMEM((2, block, rank), bf16),
            pltpu.VMEM((2, block, columns), f32),
            pltpu.VMEM((2, low_rows, columns), f32),
            pltpu.VMEM((2, low_rows, columns), f32),
            pltpu.VMEM((2, n, part, block), bf16),
            pltpu.VMEM((2, n, block // CHUNKS, columns), bf16),
            pltpu.VMEM((2, m, n, part, block // CHUNKS), bf16),
            pltpu.VMEM((2, n, block // CHUNKS, rank), bf16),
            pltpu.VMEM((2, m, 2, part, tokens), bf16),
            pltpu.VMEM((2, n, low_rows, columns), f32),
            pltpu.VMEM((2, n // 2, low_rows, columns), f32),
            pltpu.VMEM((2, n // 2, low_rows, columns), f32),
            pltpu.VMEM((n * m, 8, 128), f32),
            pltpu.VMEM((2, n, low_rows, columns), bf16),
            dma((6, 2)),
            dma((2, 2, n)),
            dma((2, 2, m)),
            dma((2, 2, n // 2)),
            dma((2, 2, n // 2)),
            dma((2, n * m)),
            dma((2, 2, n)),
            dma((2, 2, n - 1, CHUNKS)),
            dma((2, 2, n)),
            dma((2, 2, m)),
        ],
        compiler_params=pltpu.CompilerParams(
            collective_id=0, has_side_effects=True, vmem_limit_bytes=48 * 2**20
        ),
    )(*args)
    return pl.pallas_call(
        functools.partial(write_kernel, len(kinds)),
        out_shape=tuple(jax.ShapeDtypeStruct(*kind) for kind in kinds),
        in_specs=[pl.BlockSpec(memory_space=pl.ANY)] * len(kinds),
        out_specs=(hbm,) * len(kinds),
        scratch_shapes=[dma((len(kinds),))],
        compiler_params=pltpu.CompilerParams(vmem_limit_bytes=2**20),
    )(*results)


def fits(n, m, *args):
    basis, first = args[4], args[8]
    return (
        n % 2 == 0
        and basis.shape[1] // n % 16 == 0
        and basis.shape[1] // m % 16 == 0
        and basis.shape[0] // n % (128 * CHUNKS) == 0
        and basis.shape[0] // n % 128 == 0
        and first.shape[1] // m % 128 == 0
    )


def solution(mesh):
    placed = (
        P("fs", None),
        P("fs", "tp"),
        P("fs", None),
        P("fs", "tp"),
        P("fs", None),
        P("fs", None),
        P("fs", "tp"),
        P("fs", "tp"),
        P("fs", "tp"),
        P("fs", "tp"),
        P("fs", "tp"),
        P("fs", "tp"),
    )
    n, m = mesh.shape["fs"], mesh.shape["tp"]

    def step(*args):
        body = functools.partial(fused_per_device, n, m) if fits(n, m, *args) else per_device
        return jax.shard_map(
            body,
            mesh=mesh,
            in_specs=placed,
            out_specs=(P("fs", "tp"),) * 8 + (P(None, "tp"),) * 2,
            check_vma=False,
        )(*args)

    return step
```

```python
import functools

import jax
import jax.numpy as jnp
from jax import lax
from jax.experimental import pallas as pl
from jax.experimental.pallas import tpu as pltpu
from jax.sharding import PartitionSpec as P

QW = 2048
RANK = 256


beta_one = 0.8
beta_two = 0.9
rate = 0.1


def moment_update(low, factor, first, second):
    scaled = low * factor
    first_new = beta_one * first + (1.0 - beta_one) * scaled
    second_new = beta_two * second + (1.0 - beta_two) * scaled * scaled
    direction = (first_new / jnp.sqrt(second_new)).astype(jnp.bfloat16)
    return (first_new, second_new, direction)


def contract_tokens(left, right):
    return lax.dot_general(
        left,
        right,
        (((0,), (0,)), ((), ())),
        precision=lax.Precision.HIGHEST,
        preferred_element_type=jnp.float32,
    )


def per_device(
    saved_input,
    query_cotangent,
    layer_cotangent,
    mixed_heads,
    query_basis,
    output_basis,
    query_master,
    output_master,
    query_first,
    query_second,
    output_first,
    output_second,
):
    query_coords = jnp.dot(
        saved_input,
        lax.all_gather(query_basis, "fs", axis=0, tiled=True),
        preferred_element_type=jnp.float32,
    )
    output_coords = jnp.dot(
        layer_cotangent,
        lax.all_gather(output_basis, "fs", axis=0, tiled=True),
        preferred_element_type=jnp.float32,
    )
    query_part = contract_tokens(query_coords, query_cotangent.astype(jnp.float32))
    output_part = contract_tokens(output_coords, mixed_heads.astype(jnp.float32))
    query_low, output_low = (
        lax.psum_scatter(query_part, "fs", scatter_dimension=0, tiled=True),
        lax.psum_scatter(output_part, "fs", scatter_dimension=0, tiled=True),
    )
    local_squares = jnp.sum(query_low * query_low) + jnp.sum(output_low * output_low)
    total_squares = lax.psum(local_squares, ("fs", "tp"))
    factor = 1.0 / jnp.sqrt(1.0 + total_squares / (2.0 * RANK * QW))
    qf, qs, qdir = moment_update(query_low, factor, query_first, query_second)
    of, osec, odir = moment_update(output_low, factor, output_first, output_second)
    query_whole, output_whole = (
        lax.all_gather(qdir, "fs", axis=0, tiled=True),
        lax.all_gather(odir, "fs", axis=0, tiled=True),
    )
    query_step = jnp.dot(query_basis, query_whole, preferred_element_type=jnp.float32)
    output_step = jnp.dot(output_basis, output_whole, preferred_element_type=jnp.float32)
    query_weight = query_master - rate * query_step
    output_weight = output_master - rate * output_step
    query_copy, output_copy = (
        lax.all_gather(query_weight.astype(jnp.bfloat16), "fs", axis=0, tiled=True),
        lax.all_gather(output_weight.astype(jnp.bfloat16), "fs", axis=0, tiled=True),
    )
    return (
        query_weight,
        output_weight,
        query_step,
        output_step,
        qf,
        qs,
        of,
        osec,
        query_copy,
        output_copy,
    )

MESH = pl.DeviceIdType.MESH
CHUNKS = 4


def ring_kernel(n, m, *refs):
    x_hbm, cot_hbm, basis_hbm, master_hbm, first_hbm, second_hbm = (
        (refs[0], refs[2]),
        (refs[1], refs[3]),
        (refs[4], refs[5]),
        (refs[6], refs[7]),
        (refs[8], refs[10]),
        (refs[9], refs[11]),
    )
    w_out, step_out, first_out, second_out, gathered = (
        (refs[12], refs[13]),
        (refs[14], refs[15]),
        (refs[16], refs[18]),
        (refs[17], refs[19]),
        (refs[20], refs[21]),
    )
    (
        x_v, cot_v, basis, master_v, first, second,
        rows_v, ahead_v, wide_v, flat_v, coord_v, part_v, pair_v, got_v, square_v, direction_v,
        in_sem, rows_sem, coord_sem, pair_sem, part_sem, square_sem, direction_sem, gather_sem, ahead_sem, wide_sem,
    ) = refs[22:]
    f, t = lax.axis_index("fs"), lax.axis_index("tp")
    me = f * m + t
    rank_part, block = rows_v.shape[2:]
    piece = block // CHUNKS
    rank = basis.shape[2]
    tokens = x_v.shape[1]
    columns = cot_v.shape[2]
    low_rows = first.shape[1]
    half = n // 2
    z, x = f // 2, lax.rem(f, 2)
    across = z * 2 + 1 - x

    def along(d, side=None):
        side = x if side is None else side
        return lax.rem(z + d + half, half) * 2 + side

    loads = {}
    for k in range(2):
        loads["basis", k] = pltpu.make_async_copy(basis_hbm[k], basis.at[k], in_sem.at[0, k])
    for i, (name, sources, target) in enumerate(
        (
            ("x", x_hbm, x_v),
            ("cot", cot_hbm, cot_v),
            ("first", first_hbm, first),
            ("second", second_hbm, second),
            ("master", master_hbm, master_v),
        )
    ):
        for k in range(2):
            loads[name, k] = pltpu.make_async_copy(sources[k], target.at[k], in_sem.at[1 + i, k])
    for copy in loads.values():
        copy.start()

    barrier = pltpu.get_barrier_semaphore()
    for d in range(1, n * m):
        other = lax.rem(me + d, n * m)
        pl.semaphore_signal(barrier, inc=1, device_id={"fs": other // m, "tp": lax.rem(other, m)}, device_id_type=MESH)

    chosen = lax.broadcasted_iota(jnp.int32, (rank_part, rank), 1) == (
        lax.broadcasted_iota(jnp.int32, (rank_part, rank), 0) + t * rank_part
    )
    select = jnp.where(chosen, 1.0, 0.0).astype(jnp.bfloat16)
    for k in range(2):
        loads["basis", k].wait()
        rows_v[k, 0] = lax.dot_general(
            select, basis[k], (((1,), (1,)), ((), ())), preferred_element_type=jnp.float32
        ).astype(jnp.bfloat16)
    pl.semaphore_wait(barrier, n * m - 1)

    sent = []

    def send(source, target, sems, index, device):
        copy = pltpu.make_async_remote_copy(
            src_ref=source,
            dst_ref=target,
            send_sem=sems.at[(0,) + index],
            recv_sem=sems.at[(1,) + index],
            device_id=device,
            device_id_type=MESH,
        )
        copy.start()
        sent.append(copy)
        return copy

    def push(own, slots, sems, k):
        copies = {half: send(own, slots(half), sems, (k, half), {"fs": across})}
        for d in (1, half - 1, *range(2, half - 1)):
            copies[d] = send(own, slots(d), sems, (k, d), {"fs": along(d)})
        return copies

    def relay(copies, slots, sems, k):
        for d in (1, half - 1, *range(2, half - 1)):
            copies[d].wait_recv()
            copies[half + d] = send(slots(d), slots(half + d), sems, (k, half + d), {"fs": across})

    def rows_at(k):
        return lambda d: rows_v.at[k, d]

    rows = [push(rows_v.at[k, 0], rows_at(k), rows_sem, k) for k in range(2)]

    def coordinates(k, d):
        source = along(-(d % half), x if d < half else 1 - x)
        left = rows_v[k, d]
        right = x_v[k, :, pl.ds(pl.multiple_of(source * block, block), block)]
        return lax.dot_general(left, right, (((1,), (1,)), ((), ())), preferred_element_type=jnp.float32)

    def ahead_at(k):
        return lambda d: ahead_v.at[k, d]

    coords, ahead = [], []
    for k in range(2):
        if k == 0:
            relay(rows[0], rows_at(0), rows_sem, 0)
        loads["x", k].wait()
        total = coordinates(k, 0)
        for d in range(1, half):
            total = total + coordinates(k, d)
        if k == 0:
            relay(rows[1], rows_at(1), rows_sem, 1)
            for i in range(2):
                loads["master", i].wait()
                ahead_v[i, 0] = master_v[i, pl.ds(0, piece)].astype(jnp.bfloat16)
                ahead.append(push(ahead_v.at[i, 0], ahead_at(i), ahead_sem, i))
        for d in range(half, n):
            rows[k][d].wait_recv()
            total = total + coordinates(k, d)
        high = total.astype(jnp.bfloat16)
        coord_v[k, t, 0] = high
        coord_v[k, t, 1] = (total - high.astype(jnp.float32)).astype(jnp.bfloat16)
        coords.append(
            [
                send(coord_v.at[k, t], coord_v.at[k, t], coord_sem, (k, d), {"tp": lax.rem(t + d, m)})
                for d in range(1, m)
            ]
        )

    wide = []
    for k in range(2):
        source = rows_v.at[k, :, :, pl.ds(0, piece)]
        for d in range(1, m):
            wide.append(send(source, wide_v.at[k, t], wide_sem, (k, d), {"tp": lax.rem(t + d, m)}))
        wide_v[k, t] = rows_v[k, :, :, :piece]
    pairs = []
    for k in range(2):
        loads["cot", k].wait()
        for copy in coords[k]:
            copy.wait_recv()
        part = jnp.dot(
            coord_v[k, :, 0].reshape(rank, tokens), cot_v[k], preferred_element_type=jnp.float32
        ) + jnp.dot(coord_v[k, :, 1].reshape(rank, tokens), cot_v[k], preferred_element_type=jnp.float32)
        part_v[k] = part.reshape(n, low_rows, columns)
        pairs.append({})
        for d in (1, half - 1, *range(2, half - 1), 0):
            pairs[k][d] = send(
                part_v.at[k, along(d, 1 - x)], pair_v.at[k, d], pair_sem, (k, d), {"fs": across}
            )
    parts = []
    for k in range(2):
        parts.append({})
        for d in (1, half - 1, *range(2, half - 1)):
            pairs[k][d].wait_recv()
            pair_v[k, d] = pair_v[k, d] + part_v[k, along(d)]
            parts[k][d] = send(pair_v.at[k, d], got_v.at[k, d], part_sem, (k, d), {"fs": along(d)})
        relay(ahead[k], ahead_at(k), ahead_sem, k)

    lows = []
    squares = jnp.zeros((), jnp.float32)
    for k in range(2):
        pairs[k][0].wait_recv()
        low = pair_v[k, 0] + part_v[k, f]
        for d in range(1, half):
            parts[k][d].wait_recv()
            low = low + got_v[k, d]
        lows.append(low)
        squares = squares + jnp.sum(low * low)
    square_v[0] = jnp.full(square_v.shape[1:], squares, jnp.float32)
    copies = []
    for d in range(1, n * m):
        other = lax.rem(me + d, n * m)
        copies.append(
            send(square_v.at[0], square_v.at[d], square_sem, (d,), {"fs": other // m, "tp": lax.rem(other, m)})
        )
    for copy in wide:
        copy.wait_recv()
    for k in range(2):
        for d in range(n):
            flat_v[k, d] = wide_v[k, :, d].reshape(rank, piece).T
    for k in range(2):
        loads["first", k].wait()
        loads["second", k].wait()
    for copy in copies:
        copy.wait_recv()
    total_squares = jnp.sum(square_v[...], axis=0)[:1, :1]
    factor = 1.0 / jnp.sqrt(1.0 + total_squares / (2.0 * rank * (columns * m)))

    directions = []
    for k in range(2):
        new_first, new_second, direction = moment_update(lows[k], factor, first[k], second[k])
        direction_v[k, f] = direction
        own = direction_v.at[k, f]
        directions.append(push(own, lambda d: own, direction_sem, k))
        first_out[k][...] = new_first
        second_out[k][...] = new_second
    for k in range(2):
        for d in (1, half - 1, *range(2, half - 1)):
            directions[k][d].wait_recv()
            arrived = direction_v.at[k, along(-d)]
            directions[k][half + d] = send(arrived, arrived, direction_sem, (k, half + d), {"fs": across})

    place = (1 - x) * z + x * (n - 1 - z)

    def at(p):
        p = lax.rem(p + 2 * n, n)
        h = p // half
        return (1 - h) * 2 * p + h * (2 * (n - 1 - p) + 1)

    toward = (at(place + 1), at(place - 1))
    origin = [[at(place - s), at(place + s)] for s in range(n)]
    for k in range(2):
        for d in range(half, n):
            directions[k][d].wait_recv()
    ring = {}

    def forward(s, k, c):
        where = gathered[k].at[pl.ds(pl.multiple_of(origin[s][k] * block + c * piece, piece), piece)]
        ring[s, k, c] = send(where, where, gather_sem, (k, s, c), {"fs": toward[k]})

    def own_piece(c):
        for k in range(2):
            span = pl.ds(c * piece, piece)
            step = jnp.dot(
                basis[k, span, :],
                direction_v[k].reshape(rank, columns),
                preferred_element_type=jnp.float32,
            )
            weight = master_v[k, span, :] - rate * step
            if c > 0:
                gathered[k][pl.ds(pl.multiple_of(f * block + c * piece, piece), piece)] = weight.astype(jnp.bfloat16)
                forward(0, k, c)
            step_out[k][span] = step
            w_out[k][span] = weight
    def finish_ahead(k, d):
        source = along(-(d % half), x if d < half else 1 - x)
        if d >= half:
            ahead[k][d].wait_recv()
        step = jnp.dot(
            flat_v[k, d], direction_v[k].reshape(rank, columns), preferred_element_type=jnp.float32
        )
        weight = ahead_v[k, d].astype(jnp.float32) - rate * step
        gathered[k][pl.ds(pl.multiple_of(source * block, block), piece)] = weight.astype(jnp.bfloat16)

    for c in (*range(1, CHUNKS), 0):
        own_piece(c)
    units = [(k, d) for d in range(n) for k in range(2)]
    for s in range(1, n):
        for c in range(1, CHUNKS):
            for k in range(2):
                ring[s - 1, k, c].wait_recv()
                if s < n - 1:
                    forward(s, k, c)
            if units:
                finish_ahead(*units.pop(0))
    for unit in units:
        finish_ahead(*unit)
    for copy in sent:
        copy.wait_send()


def write_kernel(count, *refs):
    sem = refs[2 * count]
    copies = [pltpu.make_async_copy(refs[i], refs[count + i], sem.at[i]) for i in range(count)]
    for copy in copies:
        copy.start()
    for copy in copies:
        copy.wait()


def fused_per_device(n, m, *args):
    x, cot, _, _, basis = args[:5]
    first = args[8]
    block, rank = basis.shape
    columns = cot.shape[1]
    tokens, width = x.shape
    part = rank // m
    low_rows = first.shape[0]
    bf16, f32 = jnp.bfloat16, jnp.float32
    kinds = [((block, columns), f32)] * 4 + [(first.shape, f32)] * 4 + [((width, columns), bf16)] * 2
    hbm = pl.BlockSpec(memory_space=pltpu.HBM)
    vmem = pl.BlockSpec(memory_space=pltpu.VMEM)
    dma = pltpu.SemaphoreType.DMA
    results = pl.pallas_call(
        functools.partial(ring_kernel, n, m),
        out_shape=tuple(pltpu.VMEM(*kind) for kind in kinds),
        in_specs=[hbm] * 12,
        out_specs=(vmem,) * 10,
        scratch_shapes=[
            pltpu.VMEM((2, tokens, width), bf16),
            pltpu.VMEM((2, tokens, columns), bf16),
            pltpu.VMEM((2, block, rank), bf16),
            pltpu.VMEM((2, block, columns), f32),
            pltpu.VMEM((2, low_rows, columns), f32),
            pltpu.VMEM((2, low_rows, columns), f32),
            pltpu.VMEM((2, n, part, block), bf16),
            pltpu.VMEM((2, n, block // CHUNKS, columns), bf16),
            pltpu.VMEM((2, m, n, part, block // CHUNKS), bf16),
            pltpu.VMEM((2, n, block // CHUNKS, rank), bf16),
            pltpu.VMEM((2, m, 2, part, tokens), bf16),
            pltpu.VMEM((2, n, low_rows, columns), f32),
            pltpu.VMEM((2, n // 2, low_rows, columns), f32),
            pltpu.VMEM((2, n // 2, low_rows, columns), f32),
            pltpu.VMEM((n * m, 8, 128), f32),
            pltpu.VMEM((2, n, low_rows, columns), bf16),
            dma((6, 2)),
            dma((2, 2, n)),
            dma((2, 2, m)),
            dma((2, 2, n // 2)),
            dma((2, 2, n // 2)),
            dma((2, n * m)),
            dma((2, 2, n)),
            dma((2, 2, n - 1, CHUNKS)),
            dma((2, 2, n)),
            dma((2, 2, m)),
        ],
        compiler_params=pltpu.CompilerParams(
            collective_id=0, has_side_effects=True, vmem_limit_bytes=48 * 2**20
        ),
    )(*args)
    return pl.pallas_call(
        functools.partial(write_kernel, len(kinds)),
        out_shape=tuple(jax.ShapeDtypeStruct(*kind) for kind in kinds),
        in_specs=[pl.BlockSpec(memory_space=pl.ANY)] * len(kinds),
        out_specs=(hbm,) * len(kinds),
        scratch_shapes=[dma((len(kinds),))],
        compiler_params=pltpu.CompilerParams(vmem_limit_bytes=2**20),
    )(*results)


def fits(n, m, *args):
    basis, first = args[4], args[8]
    return (
        n % 2 == 0
        and basis.shape[1] // n % 16 == 0
        and basis.shape[1] // m % 16 == 0
        and basis.shape[0] // n % (128 * CHUNKS) == 0
        and basis.shape[0] // n % 128 == 0
        and first.shape[1] // m % 128 == 0
    )


def solution(mesh):
    placed = (
        P("fs", None),
        P("fs", "tp"),
        P("fs", None),
        P("fs", "tp"),
        P("fs", None),
        P("fs", None),
        P("fs", "tp"),
        P("fs", "tp"),
        P("fs", "tp"),
        P("fs", "tp"),
        P("fs", "tp"),
        P("fs", "tp"),
    )
    n, m = mesh.shape["fs"], mesh.shape["tp"]

    def step(*args):
        body = functools.partial(fused_per_device, n, m) if fits(n, m, *args) else per_device
        return jax.shard_map(
            body,
            mesh=mesh,
            in_specs=placed,
            out_specs=(P("fs", "tp"),) * 8 + (P(None, "tp"),) * 2,
            check_vma=False,
        )(*args)

    return step
```
